32 devices in a mesh: ep: 8 (over z, x), tp: 4 (over y, core).
Axes of the slice: x: 2, y: 2, z: 4, core: 2. Of those that a mesh axis runs over, the one named last changes fastest.
Arguments:
- tokens: bfloat16 [1024, 2048], P('ep'), may hold values from -6 to 6
- routing: int32 [1024, 2], P('ep'), may hold values from 0 to 7, all different within a row; in each aligned block of 128 rows (0 to 127, 128 to 255, ...) at most 56 rows name the same one
- router_weight: bfloat16 [2048, 8], replicated, may hold values from -0.125 to 0.125
- gate_weight: bfloat16 [8, 2048, 2048], P('ep', None, 'tp'), may hold values from -0.125 to 0.125
- up_weight: bfloat16 [8, 2048, 2048], P('ep', None, 'tp'), may hold values from -0.125 to 0.125
- down_weight: bfloat16 [8, 2048, 2048], P('ep', 'tp'), may hold values from -0.125 to 0.125
- cotangent: bfloat16 [1024, 2048], P('ep'), may hold values from -0.796875 to 0.796875
Outputs:
- token_grad: bfloat16 [1024, 2048], P('ep')
- router_grad: float32 [2048, 8], P('tp')
- router_rows: float32 [2048], P('tp')
- gate_grad: bfloat16 [8, 2048, 2048], P('ep', None, 'tp')
- up_grad: bfloat16 [8, 2048, 2048], P('ep', None, 'tp')
- down_grad: bfloat16 [8, 2048, 2048], P('ep', 'tp')
- gate_rows: float32 [8, 2048], P('ep')
- up_rows: float32 [8, 2048], P('ep')
- down_rows: float32 [8, 2048], P('ep', 'tp')
The draws below stay inside these ranges and needn't reach their ends.
Inputs may be any that keep to these rules, and one draw needn't show every extreme that they name: `routing`: A row's 2 experts differ. Within the rows of one index of ep (128 rows), no expert is named more than 56 times, a bound that some block reaches.
All inputs are finite; a program needn't handle non-finite values.
Results may differ from the reference program's by a relative error of at most 0.01.
Values may be sent and summed in bfloat16 or wider, within the bound.
A program may use at most 64 MiB of HBM per device.

```python
import math
import jax
import jax.numpy as jnp
import numpy as np
from jax import lax

D = 2048
FF = 2048
TOPK = 2
TOK_DEV = 128
EXPERTS = 8
TOKENS = 1024
CAP = 56
N_EP = 8


def level_of(stream_key, shape, pieces, low, high):
    gain = 1.0
    for axis_at, parts in pieces:
        steps = jax.random.uniform(jax.random.fold_in(jax.random.fold_in(stream_key, 6), axis_at), (parts,), jnp.float32, low / len(pieces), high / len(pieces))
        gain = gain * jnp.repeat(jnp.exp(steps), shape[axis_at] // parts).reshape((-1,) + (1,) * (len(shape) - 1 - axis_at))
    return gain


def shared_out(rng, own, number, rows, number_of, top, most, lean):
    sequence = jax.random.permutation(rng, number_of)
    crowded, common = shares(number_of, rows * top, most, lean, True), shares(number_of, rows * top, most, lean, False)
    places = jnp.arange(number_of)

    def named(lengths, turn):
        used = int((lengths > 0).sum())
        fixed = max(1, used // 4)
        moved = fixed + (places - fixed + turn * (used - fixed)) % max(1, number_of - fixed)
        return jnp.zeros((number_of,), jnp.int32).at[sequence[jnp.where(places < fixed, places, moved)]].set(jnp.asarray(lengths, jnp.int32))

    lengths = jnp.where(number % 4 == 0, named(crowded, number // 4), named(common, number - number // 4 - 1))
    mixed = jax.random.permutation(jax.random.fold_in(own, 3), number_of)
    donor, sink = mixed[0:number_of // 2 * 2:2], mixed[1:number_of // 2 * 2:2]
    room = jnp.minimum(lengths[donor] - 1, most - lengths[sink]) // 2
    room = jnp.where((donor == sequence[0]) | (sink == sequence[0]) | (lengths[sink] == 0), 0, jnp.maximum(room, 0))
    moved = jax.random.randint(jax.random.fold_in(own, 4), (number_of // 2,), 0, 1 << 20) % (room + 1)
    lengths = lengths.at[donor].add(-moved).at[sink].add(moved)
    members = jnp.searchsorted(jnp.cumsum(lengths), jnp.arange(rows * top), side="right").astype(jnp.int32)
    grid = members.reshape(top, rows).T
    grid = grid[jax.random.permutation(jax.random.fold_in(own, 1), rows)]
    turn = jax.random.randint(jax.random.fold_in(own, 2), (rows, 1), 0, top)
    return jnp.take_along_axis(grid, (jnp.arange(top)[None, :] + turn) % top, axis=1)


def shares(number_of, total, bound, lean, full):
    portions = [(1 << 20) // math.isqrt(standing ** lean) + 1 for standing in range(1, number_of + 1)]
    largest = bound if full else min(bound, max(-(-total // number_of), total * portions[0] // sum(portions)))
    least = 1 if total - largest >= number_of - 1 else 0
    holding, spare = [largest] + [least] * (number_of - 1), total - largest - least * (number_of - 1)
    while spare > 0:
        candidates = [i for i in range(1, number_of) if holding[i] < largest] or [i for i in range(1, number_of) if holding[i] < bound]
        whole, left = sum([portions[i] for i in candidates]), spare
        for i in candidates:
            extra = min(bound - holding[i], max(1, left * portions[i] // whole), spare)
            holding[i] = holding[i] + extra
            spare = spare - extra
    return np.array(holding)


def gaussian(stream_key, extent, width, reach, split=(), held_as=jnp.bfloat16):
    drawn = width * jax.random.normal(stream_key, extent, jnp.float32)
    if split:
        drawn = drawn * level_of(stream_key, extent, split, -0.22, 0.18)
    return jnp.clip(drawn, -reach, reach).astype(held_as)


def setup_inputs(seed: int = 0) -> dict:
    keys = jax.random.split(jax.random.key(seed), 8)
    tokens = gaussian(keys[0], (TOKENS, D), 1.0, 6.0, ((0, 8),))
    routing_keys = jax.random.split(jax.random.fold_in(keys[1], 1), TOKENS // TOK_DEV)
    routing_turns = jax.random.permutation(jax.random.fold_in(keys[1], 3), TOKENS // TOK_DEV)
    routing = jax.vmap(lambda own, number: shared_out(jax.random.fold_in(keys[1], 2), own, number, TOK_DEV, EXPERTS, TOPK, CAP, 2))(routing_keys, routing_turns).reshape((TOKENS, TOPK))
    router_weight = gaussian(keys[2], (D, EXPERTS), D ** -0.5, 0.125)
    gate_weight = gaussian(keys[3], (EXPERTS, D, FF), D ** -0.5, 0.125, ((0, 8), (2, 4)))
    up_weight = gaussian(keys[4], (EXPERTS, D, FF), D ** -0.5, 0.125, ((0, 8), (2, 4)))
    down_weight = gaussian(keys[5], (EXPERTS, FF, D), FF ** -0.5, 0.125, ((0, 8), (1, 4)))
    cotangent = gaussian(keys[6], (TOKENS, D), 0.1, 0.796875, ((0, 8),))
    return dict(tokens=tokens, routing=routing, router_weight=router_weight, gate_weight=gate_weight, up_weight=up_weight, down_weight=down_weight, cotangent=cotangent)


def block_slots(route_block):
    flat_ids = route_block.reshape(-1)
    onehot = (flat_ids[:, None] == jnp.arange(EXPERTS, dtype=jnp.int32)[None, :]).astype(jnp.int32)
    position = jnp.sum((jnp.cumsum(onehot, axis=0) - 1) * onehot, axis=1)
    return flat_ids, position.astype(jnp.int32)


def expert_backward(rows_in, cots_in, slot_scale, w_gate, w_up, w_down):
    pre_gate = jnp.dot(rows_in, w_gate, preferred_element_type=jnp.float32)
    pre_up = jnp.dot(rows_in, w_up, preferred_element_type=jnp.float32)
    sigmoid_gate = jax.nn.sigmoid(pre_gate)
    hidden = (pre_gate * sigmoid_gate * pre_up).astype(jnp.bfloat16)
    back_proj = lax.dot_general(cots_in, w_down, (((1,), (1,)), ((), ())), preferred_element_type=jnp.float32)
    gate_term = jnp.sum(hidden.astype(jnp.float32) * back_proj, axis=1)
    scaled = slot_scale * back_proj
    grad_up_pre = (scaled * pre_gate * sigmoid_gate).astype(jnp.bfloat16)
    grad_gate_pre = (scaled * pre_up * sigmoid_gate * (1.0 + pre_gate * (1.0 - sigmoid_gate))).astype(jnp.bfloat16)
    weighted = (slot_scale * cots_in.astype(jnp.float32)).astype(jnp.bfloat16)
    contract_rows = (((0,), (0,)), ((), ()))
    grad_down = lax.dot_general(hidden, weighted, contract_rows, preferred_element_type=jnp.float32)
    grad_gate = lax.dot_general(rows_in, grad_gate_pre, contract_rows, preferred_element_type=jnp.float32)
    grad_up = lax.dot_general(rows_in, grad_up_pre, contract_rows, preferred_element_type=jnp.float32)
    contract_hidden = (((1,), (1,)), ((), ()))
    partial_value = lax.dot_general(grad_gate_pre, w_gate, contract_hidden, preferred_element_type=jnp.float32)
    partial_value = partial_value + lax.dot_general(grad_up_pre, w_up, contract_hidden, preferred_element_type=jnp.float32)
    return partial_value, gate_term, grad_gate, grad_up, grad_down


def reference(tokens, routing, router_weight, gate_weight, up_weight, down_weight, cotangent):
    logits = jnp.dot(tokens, router_weight, preferred_element_type=jnp.float32)
    affinity = jax.nn.sigmoid(logits)
    chosen = jnp.take_along_axis(affinity, routing, axis=1)
    total_aff = jnp.sum(chosen, axis=1, keepdims=True)
    weights = chosen / total_aff
    assigns = TOKENS * TOPK
    flat_ids, positions = jax.vmap(block_slots)(routing.reshape(N_EP, TOK_DEV, TOPK))
    source = jnp.arange(N_EP, dtype=jnp.int32)[:, None]
    slot_index = ((flat_ids * N_EP + source) * CAP + positions).reshape(-1)
    slot_table = jnp.full((EXPERTS * N_EP * CAP,), assigns, jnp.int32)
    slot_table = slot_table.at[slot_index].set(jnp.arange(assigns, dtype=jnp.int32))
    slot_table = slot_table.reshape(EXPERTS, N_EP * CAP)
    zero_row = jnp.zeros((1, D), jnp.bfloat16)
    tok_pad = jnp.concatenate([tokens, zero_row], axis=0)
    cot_pad = jnp.concatenate([cotangent, zero_row], axis=0)
    weight_pad = jnp.concatenate([weights.astype(jnp.bfloat16).reshape(-1), jnp.zeros((1,), jnp.bfloat16)])

    def expert(operands):
        slot_ids, w_gate, w_up, w_down = operands
        rows_in = tok_pad[slot_ids // TOPK]
        cots_in = cot_pad[slot_ids // TOPK]
        slot_scale = weight_pad[slot_ids].astype(jnp.float32)[:, None]
        return expert_backward(rows_in, cots_in, slot_scale, w_gate, w_up, w_down)

    partial_value, gate_term, grad_gate, grad_up, grad_down = lax.map(expert, (slot_table, gate_weight, up_weight, down_weight))
    gate_rows = jnp.sum(grad_gate * grad_gate, axis=2)
    up_rows = jnp.sum(grad_up * grad_up, axis=2)
    down_rows = jnp.sum(grad_down * grad_down, axis=2)
    flat_table = slot_table.reshape(-1)
    slot_grad = jnp.zeros((assigns + 1, D), jnp.bfloat16).at[flat_table].set(partial_value.astype(jnp.bfloat16).reshape(-1, D))
    slot_gate = jnp.zeros((assigns + 1,), jnp.bfloat16).at[flat_table].set(gate_term.astype(jnp.bfloat16).reshape(-1))
    back_rows = jnp.sum(slot_grad[:assigns].astype(jnp.float32).reshape(TOKENS, TOPK, D), axis=1)
    d_weights = slot_gate[:assigns].astype(jnp.float32).reshape(TOKENS, TOPK)
    d_chosen = (d_weights - jnp.sum(d_weights * weights, axis=1, keepdims=True)) / total_aff
    d_logit = d_chosen * chosen * (1.0 - chosen)
    onehot = (routing[:, :, None] == jnp.arange(EXPERTS, dtype=jnp.int32)[None, None, :]).astype(jnp.float32)
    d_logits = jnp.sum(d_logit[:, :, None] * onehot, axis=1).astype(jnp.bfloat16)
    router_grad = lax.dot_general(tokens, d_logits, (((0,), (0,)), ((), ())), preferred_element_type=jnp.float32)
    router_rows = jnp.sum(router_grad * router_grad, axis=1)
    router_back = lax.dot_general(d_logits, router_weight, (((1,), (1,)), ((), ())), preferred_element_type=jnp.float32)
    token_grad = (back_rows + router_back).astype(jnp.bfloat16)
    return (token_grad, router_grad, router_rows, grad_gate.astype(jnp.bfloat16), grad_up.astype(jnp.bfloat16),
            grad_down.astype(jnp.bfloat16), gate_rows, up_rows, down_rows)
```

```python
import functools

import jax
import jax.numpy as jnp
from jax import lax
from jax.experimental import pallas as pl
from jax.experimental.pallas import tpu as pltpu
from jax.sharding import PartitionSpec as P

LANES = 128
F32 = jnp.float32
BF16 = jnp.bfloat16
ROWS_T = (((0,), (0,)), ((), ()))
COLS_T = (((1,), (1,)), ((), ()))


def barrier(n_ep, n_tp, me, tp):
    sem = pltpu.get_barrier_semaphore()
    for i in range(1, n_ep):
        pl.semaphore_signal(sem, inc=1, device_id={"ep": lax.rem(me + i, n_ep)})
    for i in range(1, n_tp):
        pl.semaphore_signal(sem, inc=1, device_id={"tp": lax.rem(tp + i, n_tp)})
    pl.semaphore_wait(sem, n_ep + n_tp - 2)


def remote(src, dst, send, recv, where):
    return pltpu.make_async_remote_copy(
        src_ref=src, dst_ref=dst, send_sem=send, recv_sem=recv, device_id=where
    )


def lane_sum(value):
    total = value[:, :LANES]
    for at in range(LANES, value.shape[1], LANES):
        total = total + value[:, at : at + LANES]
    return total


def flip(index, step):
    out, bit = index, 1
    while bit <= step:
        if step & bit:
            out = out + bit - 2 * bit * lax.rem(index // bit, 2)
        bit *= 2
    return out


def moe_kernel(
    dims, tok_ref, cot_ref, routing_ref, router_ref, w_gate, w_up, w_down,
    token_ref, rgrad_ref, rowsum_ref, gate_out, up_out, down_out, down_rows_ref,
    x_ref, z_ref, scale_ref, gate_v, up_v, down_v, gate_t, up_t, down_t, w_sem,
    stage, scale_stage, pick_ref, pos_ref, weight_ref,
    xt_ref, ht_ref, weighted_ref, gate_pre_ref, up_pre_ref, part_ref, term_ref, down_acc,
    r1, s1, r2, res, back, gate_in, gate_sum, gate_back, rowsq_ref, rowsq_in, rpart, rparts, tgrad,
    sc_send, sc_recv, a_send, a_recv, y_send, y_recv, p_send, p_recv,
    s1_send, s1_recv, s2_send, s2_recv, s3_send, s3_recv, gt_send, gt_recv, gb_send, gb_recv,
    rs_send, rs_recv, rp_send, rp_recv, ty_send, ty_recv, tp_send, tp_recv,
):
    n_ep, n_tp, n_batch, sent, slab, col_width, span = dims
    per = n_ep // n_batch
    rows = per * slab
    n_y = n_tp // 2
    me = lax.axis_index("ep")
    tp = lax.axis_index("tp")
    y_at, core = tp // 2, lax.rem(tp, 2)
    partner = y_at * 2 + 1 - core
    experts = router_ref.shape[0]
    tok_count, width = tok_ref.shape
    units = gate_v.shape[1]
    ins = (tok_ref, cot_ref)
    outs = (x_ref, z_ref)
    peers = [flip(me, i) for i in range(n_ep)]
    others_y = [lax.rem(y_at + j, n_y) for j in range(1, n_y)]
    others_tp = [lax.rem(tp + j, n_tp) for j in range(1, n_tp)]

    sem = pltpu.get_barrier_semaphore()
    for i in range(1, n_ep):
        pl.semaphore_signal(sem, inc=1, device_id={"ep": peers[i]})
    for other in others_tp:
        pl.semaphore_signal(sem, inc=1, device_id={"tp": other})
    weight_copies = [
        pltpu.make_async_copy(src.at[0], dst, w_sem.at[n])
        for n, (src, dst) in enumerate(((w_gate, gate_v), (w_up, up_v), (w_down, down_v)))
    ]
    for copy in weight_copies:
        copy.start()

    def cols(index):
        return pl.ds(pl.multiple_of(index * col_width, LANES), col_width)

    routing = routing_ref[...]
    expert_ids = lax.broadcasted_iota(jnp.int32, (experts, tok_count), 0)
    named = jnp.zeros((experts, tok_count), F32)
    for k in range(routing.shape[0]):
        named = jnp.maximum(named, (routing[k : k + 1, :] == expert_ids).astype(F32))
    earlier = (
        lax.broadcasted_iota(jnp.int32, (tok_count, tok_count), 0)
        < lax.broadcasted_iota(jnp.int32, (tok_count, tok_count), 1)
    ).astype(BF16)
    pos = jnp.dot(named.astype(BF16), earlier, preferred_element_type=F32)
    pos_ref[...] = jnp.where(named > 0.0, pos, -1.0)
    slot_ids = lax.broadcasted_iota(jnp.int32, (slab, tok_count), 0).astype(F32)

    def pick_rows(i):
        pick = (pos_ref[pl.ds(peers[i], 1), :] == slot_ids).astype(F32).astype(BF16)
        pick_ref[i // per, (i % per) * slab : (i % per + 1) * slab, :] = pick
        return pick

    def a_copy(a, i):
        return remote(
            stage.at[a, i, pl.ds(0, sent)], outs[a].at[i, pl.ds(0, sent), cols(tp)],
            a_send.at[a, i], a_recv.at[a, i], {"ep": peers[i]},
        )

    def sc_copy(i):
        return remote(scale_stage.at[i], scale_ref.at[i], sc_send.at[i], sc_recv.at[i], {"ep": peers[i]})

    token_cols = (tok_ref[:, cols(tp)], cot_ref[:, cols(tp)])
    for i in range(1, n_ep):
        pick = pick_rows(i)
        for a in range(2):
            stage[a, i] = jnp.dot(pick, token_cols[a], preferred_element_type=F32).astype(BF16)
        if i == 1:
            pl.semaphore_wait(sem, n_ep + n_tp - 2)
        for a in range(2):
            a_copy(a, i).start()
    pick = pick_rows(0)
    for a in range(2):
        outs[a][0] = jnp.dot(pick, ins[a][...], preferred_element_type=F32).astype(BF16)
        if slab > sent:
            for i in range(1, n_ep):
                outs[a][i, sent:, :] = jnp.zeros((slab - sent, width), BF16)
    if slab > sent:
        for i in range(n_ep):
            back[i, sent:, :] = jnp.zeros((slab - sent, col_width), BF16)

    logits = lax.dot_general(router_ref[...], tok_ref[...], COLS_T, preferred_element_type=F32)
    aff = jax.nn.sigmoid(logits)
    total = jnp.sum(aff * named, axis=0, keepdims=True)
    weights = aff * named / total
    weight_ref[...] = weights.astype(BF16).astype(F32)
    lanes = lax.broadcasted_iota(jnp.int32, (1, rows), 1)

    def mine_of(i):
        return (lanes >= (i % per) * slab) & (lanes < (i % per + 1) * slab)

    for i in range(n_ep):
        row = jnp.broadcast_to(weight_ref[pl.ds(peers[i], 1), :], (8, tok_count)).astype(BF16)
        scale = lax.dot_general(row, pick_ref[i // per], COLS_T, preferred_element_type=F32)
        scale = jnp.where(mine_of(i), scale[0:1], 0.0)
        if i == 0:
            scale_ref[0] = scale
        else:
            scale_stage[i] = scale
            sc_copy(i).start()

    for copy in weight_copies:
        copy.wait()
    step_rows = min(256, units)

    def turn(i, carry):
        at = pl.ds(pl.multiple_of(i * step_rows, LANES), step_rows)
        down_t[:, at] = down_v[at, :].T
        return carry

    lax.fori_loop(0, units // step_rows, turn, 0)

    def turn_wide(i, carry):
        at = pl.ds(pl.multiple_of(i * span, LANES), span)
        gate_t[:, at] = gate_v[at, :].T
        up_t[:, at] = up_v[at, :].T
        return carry

    lax.fori_loop(0, width // span, turn_wide, 0)

    def y_copy(a, i, y_to):
        ref = outs[a].at[i, pl.ds(0, sent), cols(tp)]
        return remote(ref, ref, y_send.at[a, i, y_to], y_recv.at[a, i, y_at], {"tp": y_to * 2 + core})

    def y_arrival(a, i, y_from):
        ref = outs[a].at[i, pl.ds(0, sent), cols(y_from * 2 + core)]
        return remote(ref, ref, y_send.at[a, i, y_from], y_recv.at[a, i, y_from], {"tp": y_from * 2 + core})

    def p_copy(a, i, y_of):
        ref = outs[a].at[i, pl.ds(0, sent), cols(y_of * 2 + core)]
        return remote(ref, ref, p_send.at[a, i, y_of], p_recv.at[a, i, y_of], {"tp": partner})

    def p_arrival(a, i, y_of):
        ref = outs[a].at[i, pl.ds(0, sent), cols(y_of * 2 + 1 - core)]
        return remote(ref, ref, p_send.at[a, i, y_of], p_recv.at[a, i, y_of], {"tp": partner})

    def members(j):
        return [i for i in range(j * per, (j + 1) * per) if i > 0]

    def arrive(j):
        for i in members(j):
            for a in range(2):
                a_copy(a, i).wait_recv()
                for y_to in others_y:
                    y_copy(a, i, y_to).start()
                p_copy(a, i, y_at).start()

    def relay(j):
        for i in members(j):
            for a in range(2):
                for y_from in others_y:
                    y_arrival(a, i, y_from).wait_recv()
                    p_copy(a, i, y_from).start()

    def ready(j, a):
        for i in members(j):
            for y_of in [y_at] + others_y:
                p_arrival(a, i, y_of).wait_recv()

    def compute(j):
        at = slice(j * rows, (j + 1) * rows)
        for i in members(j):
            sc_copy(i).wait_recv()
        scale = scale_ref[j * per]
        for i in range(j * per + 1, (j + 1) * per):
            scale = scale + scale_ref[i]
        scale = jnp.broadcast_to(scale, (8, rows)).T[:, 0:1]
        ready(j, 0)
        x = x_ref[j * per : (j + 1) * per].reshape(rows, width)
        pre_gate = jnp.dot(x, gate_v[...], preferred_element_type=F32)
        pre_up = jnp.dot(x, up_v[...], preferred_element_type=F32)
        xt_ref[:, at] = x.T
        ready(j, 1)
        z = z_ref[j * per : (j + 1) * per].reshape(rows, width)
        back_proj = jnp.dot(z, down_t[...], preferred_element_type=F32)
        sig = jax.nn.sigmoid(pre_gate)
        hidden = (pre_gate * sig * pre_up).astype(BF16)
        terms = lane_sum(hidden.astype(F32) * back_proj)
        term_ref[j] = jnp.sum(terms.T, axis=0, keepdims=True)
        scaled = scale * back_proj
        grad_up = (scaled * pre_gate * sig).astype(BF16)
        grad_gate = (scaled * pre_up * sig * (1.0 + pre_gate * (1.0 - sig))).astype(BF16)
        up_pre_ref[at, :] = grad_up
        gate_pre_ref[at, :] = grad_gate
        part_span = min(width, 4 * LANES)
        for c in range(0, width, part_span):
            part = jnp.dot(grad_gate, gate_t[:, c : c + part_span], preferred_element_type=F32)
            part = part + jnp.dot(grad_up, up_t[:, c : c + part_span], preferred_element_type=F32)
            part_ref[j * per : (j + 1) * per, :, c : c + part_span] = (
                part.astype(BF16).reshape(per, slab, part_span)
            )
        ht_ref[:, at] = hidden.T
        weighted_ref[at, :] = (scale * z.astype(F32)).astype(BF16)

    def group(j):
        return pl.ds(j * per, per)

    def first(j, y_to):
        return remote(
            part_ref.at[group(j), pl.ds(0, sent), cols(y_to * 2 + 1 - core)], r1.at[y_to, group(j)],
            s1_send.at[j, y_to], s1_recv.at[j, y_to], {"tp": partner},
        )

    def second(j, y_to, y_from):
        return remote(
            s1.at[y_to, group(j)], r2.at[y_from, group(j)],
            s2_send.at[j, y_to], s2_recv.at[j, y_from], {"tp": y_to * 2 + core},
        )

    def third(i):
        return remote(
            res.at[i], back.at[i, pl.ds(0, sent)], s3_send.at[i], s3_recv.at[i], {"ep": peers[i]}
        )

    def gate_part(other, slot):
        return remote(term_ref, gate_in.at[slot], gt_send.at[other], gt_recv.at[slot], {"tp": other})

    def gate_home(i):
        return remote(
            gate_sum.at[i // per], gate_back.at[i], gb_send.at[i], gb_recv.at[i], {"ep": peers[i]}
        )

    def squares(other, slot):
        return remote(rowsq_ref, rowsq_in.at[slot], rs_send.at[other], rs_recv.at[slot], {"tp": other})

    def start_return(j):
        for y_to in others_y + [y_at]:
            first(j, y_to).start()

    def reduce_core(j):
        for y_to in others_y + [y_at]:
            first(j, y_to).wait_recv()
            mine = part_ref[j * per : (j + 1) * per, :sent, cols(y_to * 2 + core)].astype(F32)
            s1[y_to, group(j)] = (mine + r1[y_to, group(j)].astype(F32)).astype(BF16)
        for y_to in others_y:
            second(j, y_to, y_at).start()

    def reduce_y(j):
        value = s1[y_at, group(j)].astype(F32)
        for y_from in others_y:
            second(j, y_from, y_from).wait_recv()
            value = value + r2[y_from, group(j)].astype(F32)
        res[group(j)] = value.astype(BF16)
        for i in members(j):
            third(i).start()
        if j == 0:
            back[0, :sent] = res[0]

    arrive(0)
    for j in range(n_batch):
        if j + 1 < n_batch:
            arrive(j + 1)
        relay(j)
        compute(j)
        start_return(j)
        if j > 0:
            reduce_core(j - 1)
        if j > 1:
            reduce_y(j - 2)
    last = n_batch - 1
    for other in others_tp:
        gate_part(other, tp).start()

    def grads(c, carry):
        at = pl.ds(pl.multiple_of(c * span, LANES), span)
        xt = xt_ref[at, :]
        for a, (pre, out) in enumerate(((gate_pre_ref, gate_out), (up_pre_ref, up_out))):
            grad = jnp.dot(xt, pre[...], preferred_element_type=F32)
            out[at, :] = grad.astype(BF16)
            rowsq_ref[a, :, at] = jnp.sum(lane_sum(grad * grad).T, axis=0, keepdims=True)
        grad = jnp.dot(ht_ref[...], weighted_ref[:, at], preferred_element_type=F32)
        down_out[:, at] = grad.astype(BF16)
        down_acc[...] += lane_sum(grad * grad)
        return carry

    down_acc[...] = jnp.zeros_like(down_acc)
    chunks = width // span
    cut = [chunks * k // 4 for k in range(5)]
    lax.fori_loop(cut[0], cut[1], grads, 0)
    if n_batch > 1:
        reduce_y(last - 1)
    reduce_core(last)
    gate = term_ref[...]
    for other in others_tp:
        gate_part(other, other).wait_recv()
        gate = gate + gate_in[other]
    gate_sum[...] = gate
    for i in range(1, n_ep):
        gate_home(i).start()
    lax.fori_loop(cut[1], cut[2], grads, 0)
    reduce_y(last)
    lax.fori_loop(cut[2], cut[4], grads, 0)
    for other in others_tp:
        squares(other, tp).start()
    down_rows_ref[...] = jnp.sum(down_acc[...].T, axis=0, keepdims=True)

    d_weights = jnp.zeros((experts, tok_count), F32)
    for i in range(n_ep):
        if i == 0:
            terms = gate_sum[0]
        else:
            gate_home(i).wait_recv()
            terms = gate_back[i]
        terms = jnp.where(mine_of(i), terms, 0.0)
        terms = jnp.broadcast_to(terms, (experts, rows)).astype(BF16)
        found = jnp.dot(terms, pick_ref[i // per], preferred_element_type=F32)
        d_weights = jnp.where(expert_ids == peers[i], found, d_weights)
    mean = jnp.sum(d_weights * weights, axis=0, keepdims=True)
    d_logits = ((d_weights - mean) / total * aff * (1.0 - aff) * named).astype(BF16)
    rpart[...] = jnp.dot(d_logits, tok_ref[:, cols(tp)], preferred_element_type=F32)

    def router_copy(i):
        return remote(rpart, rparts.at[i], rp_send.at[i], rp_recv.at[i], {"ep": peers[i]})

    for i in range(1, n_ep):
        router_copy(i).start()

    grad = lax.dot_general(d_logits, router_ref[:, cols(tp)], ROWS_T, preferred_element_type=F32)
    for j in range(n_batch):
        for i in members(j):
            third(i).wait_recv()
        home = back[j * per : (j + 1) * per].reshape(rows, col_width)
        grad = grad + lax.dot_general(pick_ref[j], home, ROWS_T, preferred_element_type=F32)
    grad = grad.astype(BF16)
    tgrad[...] = grad
    token_ref[:, cols(tp)] = grad

    def to_y(y_to):
        return remote(
            tgrad, token_ref.at[:, cols(tp)], ty_send.at[y_to], ty_recv.at[y_at], {"tp": y_to * 2 + core}
        )

    def from_y(y_from):
        ref = token_ref.at[:, cols(y_from * 2 + core)]
        return remote(ref, ref, ty_send.at[y_from], ty_recv.at[y_from], {"tp": y_from * 2 + core})

    def own_pair():
        return remote(
            tgrad, token_ref.at[:, cols(tp)], tp_send.at[y_at], tp_recv.at[y_at], {"tp": partner}
        )

    def pair(y_of):
        ref = token_ref.at[:, cols(y_of * 2 + core)]
        return remote(ref, ref, tp_send.at[y_of], tp_recv.at[y_of], {"tp": partner})

    def pair_in(y_of):
        ref = token_ref.at[:, cols(y_of * 2 + 1 - core)]
        return remote(ref, ref, tp_send.at[y_of], tp_recv.at[y_of], {"tp": partner})

    for y_to in others_y:
        to_y(y_to).start()
    own_pair().start()

    rgrad = rpart[...]
    for i in range(1, n_ep):
        router_copy(i).wait_recv()
        rgrad = rgrad + rparts[i]
    rgrad_ref[...] = rgrad
    sums = rowsq_ref[...]
    for other in others_tp:
        squares(other, other).wait_recv()
        sums = sums + rowsq_in[other]
    rowsum_ref[...] = sums

    for y_from in others_y:
        from_y(y_from).wait_recv()
        pair(y_from).start()
    for y_of in [y_at] + others_y:
        pair_in(y_of).wait_recv()
    own_pair().wait_send()
    for other in others_y:
        to_y(other).wait_send()
        pair(other).wait_send()
    for other in others_tp:
        gate_part(other, tp).wait_send()
        squares(other, tp).wait_send()
    for i in range(1, n_ep):
        sc_copy(i).wait_send()
        for a in range(2):
            a_copy(a, i).wait_send()
            for y_to in others_y:
                y_copy(a, i, y_to).wait_send()
                p_copy(a, i, y_to).wait_send()
            p_copy(a, i, y_at).wait_send()
        gate_home(i).wait_send()
        third(i).wait_send()
        router_copy(i).wait_send()
    for j in range(n_batch):
        for y_to in others_y:
            first(j, y_to).wait_send()
            second(j, y_to, y_at).wait_send()
        first(j, y_at).wait_send()


def finish_kernel(
    token_ref, router_ref, sums_ref, gate_ref, up_ref, down_ref, down_rows_ref,
    token_out, router_out, rows_out, gate_rows, up_rows, gate_out, up_out, down_out, down_rows_out, sems,
):
    copies = [
        pltpu.make_async_copy(src, dst, sems.at[n])
        for n, (src, dst) in enumerate(
            ((gate_ref, gate_out), (up_ref, up_out), (down_ref, down_out), (token_ref, token_out))
        )
    ]
    for copy in copies:
        copy.start()
    grad = router_ref[...]
    router_out[...] = grad
    rows_out[...] = jnp.sum(grad * grad, axis=0, keepdims=True)
    gate_rows[...] = sums_ref[0]
    up_rows[...] = sums_ref[1]
    down_rows_out[...] = down_rows_ref[...]
    for copy in copies:
        copy.wait()


def per_device(tokens, routing, router_weight, gate_weight, up_weight, down_weight, cotangent):
    n_ep = lax.axis_size("ep")
    n_tp = lax.axis_size("tp")
    tok_count, width = tokens.shape
    top_count = routing.shape[1]
    experts = router_weight.shape[1]
    units = gate_weight.shape[2]
    capacity = 7 * tok_count * top_count // (4 * experts)
    sent = -(-capacity // 8) * 8
    slab = -(-capacity // 16) * 16
    col_width = width // n_tp
    n_batch = min(n_ep, 4)
    n_y = n_tp // 2
    rows = n_ep // n_batch * slab
    slots = n_ep * slab
    span = 2 * LANES if width % (2 * LANES) == 0 else LANES
    dims = (n_ep, n_tp, n_batch, sent, slab, col_width, span)
    vmem = pl.BlockSpec(memory_space=pltpu.VMEM)
    hbm = pl.BlockSpec(memory_space=pltpu.HBM)
    dma = pltpu.SemaphoreType.DMA
    on_chip = pltpu.VMEM

    results = pl.pallas_call(
        functools.partial(moe_kernel, dims),
        out_shape=(
            on_chip((tok_count, width), BF16),
            on_chip((experts, col_width), F32),
            on_chip((2, 1, width), F32),
            on_chip((width, units), BF16),
            on_chip((width, units), BF16),
            on_chip((units, width), BF16),
            on_chip((1, units), F32),
        ),
        in_specs=[vmem] * 4 + [hbm] * 3,
        out_specs=(vmem,) * 7,
        scratch_shapes=[
            pltpu.VMEM((n_ep, slab, width), BF16),
            pltpu.VMEM((n_ep, slab, width), BF16),
            pltpu.VMEM((n_ep, 1, rows), F32),
            pltpu.VMEM((width, units), BF16),
            pltpu.VMEM((width, units), BF16),
            pltpu.VMEM((units, width), BF16),
            pltpu.VMEM((units, width), BF16),
            pltpu.VMEM((units, width), BF16),
            pltpu.VMEM((width, units), BF16),
            dma((3,)),
            pltpu.VMEM((2, n_ep, slab, col_width), BF16),
            pltpu.VMEM((n_ep, 1, rows), F32),
            pltpu.VMEM((n_batch, rows, tok_count), BF16),
            pltpu.VMEM((experts, tok_count), F32),
            pltpu.VMEM((experts, tok_count), F32),
            pltpu.VMEM((width, slots), BF16),
            pltpu.VMEM((units, slots), BF16),
            pltpu.VMEM((slots, width), BF16),
            pltpu.VMEM((slots, units), BF16),
            pltpu.VMEM((slots, units), BF16),
            pltpu.VMEM((n_ep, slab, width), BF16),
            pltpu.VMEM((n_batch, 1, rows), F32),
            pltpu.VMEM((units, LANES), F32),
            pltpu.VMEM((n_y, n_ep, sent, col_width), BF16),
            pltpu.VMEM((n_y, n_ep, sent, col_width), BF16),
            pltpu.VMEM((n_y, n_ep, sent, col_width), BF16),
            pltpu.VMEM((n_ep, sent, col_width), BF16),
            pltpu.VMEM((n_ep, slab, col_width), BF16),
            pltpu.VMEM((n_tp, n_batch, 1, rows), F32),
            pltpu.VMEM((n_batch, 1, rows), F32),
            pltpu.VMEM((n_ep, 1, rows), F32),
            pltpu.VMEM((2, 1, width), F32),
            pltpu.VMEM((n_tp, 2, 1, width), F32),
            pltpu.VMEM((experts, col_width), F32),
            pltpu.VMEM((n_ep, experts, col_width), F32),
            pltpu.VMEM((tok_count, col_width), BF16),
            dma((n_ep,)), dma((n_ep,)),
            dma((2, n_ep)), dma((2, n_ep)),
            dma((2, n_ep, n_y)), dma((2, n_ep, n_y)),
            dma((2, n_ep, n_y)), dma((2, n_ep, n_y)),
            dma((n_batch, n_y)), dma((n_batch, n_y)),
            dma((n_batch, n_y)), dma((n_batch, n_y)),
            dma((n_ep,)), dma((n_ep,)),
            dma((n_tp,)), dma((n_tp,)),
            dma((n_ep,)), dma((n_ep,)),
            dma((n_tp,)), dma((n_tp,)),
            dma((n_ep,)), dma((n_ep,)),
            dma((n_y,)), dma((n_y,)),
            dma((n_y,)), dma((n_y,)),
        ],
        compiler_params=pltpu.CompilerParams(
            collective_id=0, has_side_effects=True, vmem_limit_bytes=48 << 20
        ),
        name="moe",
    )(tokens, cotangent, routing.T, router_weight.T, gate_weight, up_weight, down_weight)

    (token_grad, router_grad, router_rows, gate_rows, up_rows, grad_gate, grad_up, grad_down,
     down_rows) = pl.pallas_call(
        finish_kernel,
        out_shape=(
            jax.ShapeDtypeStruct((tok_count, width), BF16),
            jax.ShapeDtypeStruct((experts, col_width), F32),
            jax.ShapeDtypeStruct((1, col_width), F32),
            jax.ShapeDtypeStruct((1, width), F32),
            jax.ShapeDtypeStruct((1, width), F32),
            jax.ShapeDtypeStruct((width, units), BF16),
            jax.ShapeDtypeStruct((width, units), BF16),
            jax.ShapeDtypeStruct((units, width), BF16),
            jax.ShapeDtypeStruct((1, units), F32),
        ),
        in_specs=[vmem] * 7,
        out_specs=(hbm, vmem, vmem, vmem, vmem, hbm, hbm, hbm, vmem),
        scratch_shapes=[dma((4,))],
        compiler_params=pltpu.CompilerParams(vmem_limit_bytes=16 << 20),
        name="finish",
    )(*results)
    return (
        token_grad,
        router_grad.T,
        router_rows[0],
        grad_gate[None],
        grad_up[None],
        grad_down[None],
        gate_rows,
        up_rows,
        down_rows,
    )


def solution(mesh):
    return jax.shard_map(
        per_device,
        mesh=mesh,
        in_specs=(
            P("ep", None),
            P("ep", None),
            P(),
            P("ep", None, "tp"),
            P("ep", None, "tp"),
            P("ep", "tp", None),
            P("ep", None),
        ),
        out_specs=(
            P("ep", None),
            P("tp", None),
            P("tp"),
            P("ep", None, "tp"),
            P("ep", None, "tp"),
            P("ep", "tp", None),
            P("ep", None),
            P("ep", None),
            P("ep", "tp"),
        ),
        check_vma=False,
    )
```
